32 devices in a mesh: sp: 8 (over z, y), tp: 4 (over x, core).
Axes of the slice: x: 2, y: 2, z: 4, core: 2. Of those that a mesh axis runs over, the one named last changes fastest.
Arguments:
- hidden_states: bfloat16 [2048, 4096], P('sp', 'tp'), may hold values from -6 to 6
- norm_gain: float32 [4096], replicated, may hold values from 0.1 to 1.9
- query_weight: bfloat16 [4096, 2048], P('sp', 'tp'), may hold values from -0.09375 to 0.09375
- key_weight: bfloat16 [4096, 2048], P('sp', 'tp'), may hold values from -0.09375 to 0.09375
- value_weight: bfloat16 [4096, 2048], P('sp', 'tp'), may hold values from -0.09375 to 0.09375
- output_gate_weight: bfloat16 [4096, 2048], P('sp', 'tp'), may hold values from -0.09375 to 0.09375
- unit_input_weight: bfloat16 [4096, 2048], P('sp', 'tp'), may hold values from -0.09375 to 0.09375
- unit_gate_weight: bfloat16 [4096, 2048], P('sp', 'tp'), may hold values from -0.09375 to 0.09375
- decay_forward: float32 [16], P('tp'), may hold values from 0 to 16
- decay_backward: float32 [16], P('tp'), may hold values from 0 to 16
- group_gain: float32 [2048], P('tp'), may hold values from 0.1 to 1.9
- group_bias: float32 [2048], P('tp'), may hold values from -3 to 3
- depth_kernel: float32 [31, 2048], P(None, 'tp'), may hold values from -7 to 7
- depth_bias: float32 [2048], P('tp'), may hold values from -3 to 3
- channel_gain: float32 [2048], P('tp'), may hold values from 0.1 to 1.9
- channel_bias: float32 [2048], P('tp'), may hold values from -3 to 3
- retention_out_weight: bfloat16 [2048, 4096], P('tp', 'sp'), may hold values from -0.09375 to 0.09375
- convolution_out_weight: bfloat16 [2048, 4096], P('tp', 'sp'), may hold values from -0.09375 to 0.09375
Outputs:
- mixed_out: bfloat16 [2048, 4096], P(('sp', 'tp'))
The draws below stay inside these ranges and needn't reach their ends.
All inputs are finite; a program needn't handle non-finite values.
Results may differ from the reference program's by a relative error of at most 0.018.
Values may be sent and summed in bfloat16 or wider, within the bound.
No kernel may reach another device: no remote copies, remote signals or barrier semaphores. Data moves between devices by JAX's collectives and lax.ppermute only.
A program may use at most 128 MiB of HBM per device.

```python
import jax
import jax.numpy as jnp
from jax import lax

D = 4096
HEADS = 16
HEAD_DIM = 128
RET_WIDTH = 2048
CONV_WIDTH = 2048
KERNEL = 31
BLOCK = 128
TOKENS = 2048
N_TP = 4


def decay_logits(key, salt):
    key_pick, key_slow, key_fast = jax.random.split(jax.random.fold_in(key, salt), 3)
    keeps_state = jax.random.uniform(key_pick, (HEADS,), jnp.float32) < 0.5
    slow_rate = jnp.exp(jax.random.uniform(key_slow, (HEADS,), jnp.float32, jnp.log(0.2), jnp.log(2.0))) / TOKENS
    fast_rate = jnp.exp(jax.random.uniform(key_fast, (HEADS,), jnp.float32, jnp.log(1.0 / 100.0), jnp.log(1.0 / 30.0)))
    decay_rate = jnp.where(keeps_state, slow_rate, fast_rate)
    return -decay_rate - jnp.log(-jnp.expm1(-decay_rate))


def draw_decay_forward(key, part):
    return decay_logits(key, 11)


def draw_decay_backward(key, part):
    return decay_logits(key, 23)


def draw_depth_kernel(key, part):
    key_tap, key_spread = jax.random.split(jax.random.fold_in(key, 5))
    channel = jnp.arange(CONV_WIDTH, dtype=jnp.float32)
    rising = jnp.exp(jnp.log(3.0) * channel / CONV_WIDTH)
    spread = jnp.exp(jax.random.uniform(key_spread, (CONV_WIDTH,), jnp.float32, 0.0, jnp.log(4.0)))
    tap_values = jnp.clip(jax.random.normal(key_tap, (KERNEL, CONV_WIDTH), jnp.float32), -3.0, 3.0)
    return tap_values * (rising * spread)[None, :] / jnp.sqrt(jnp.float32(KERNEL))


def levels(own_key, shape, cuts, least, top_value):
    gain = 1.0
    for dim, blocks in cuts:
        heights = jax.random.uniform(jax.random.fold_in(jax.random.fold_in(own_key, 6), dim), (blocks,), jnp.float32, least / len(cuts), top_value / len(cuts))
        gain = gain * jnp.repeat(jnp.exp(heights), shape[dim] // blocks).reshape((-1,) + (1,) * (len(shape) - 1 - dim))
    return gain


def bell_draw(stream_key, extent, scale, most, shards=(), kind=jnp.bfloat16):
    entries = jax.random.normal(stream_key, extent, jnp.float32) * scale
    if len(shards) > 0:
        entries = levels(stream_key, extent, shards, -0.22, 0.18) * entries
    return jnp.clip(entries, min=-most, max=most).astype(kind)


def setup_inputs(seed: int = 0) -> dict:
    key_list = jax.random.split(jax.random.key(seed), 19)
    hidden_states = bell_draw(key_list[0], (TOKENS, D), 1.0, 6.0, ((0, 8), (1, 4)))
    norm_gain = jnp.clip(1.0 + 0.18 * jax.random.normal(key_list[1], (D,), jnp.float32), 0.1, 1.9)
    query_weight = bell_draw(key_list[2], (D, RET_WIDTH), D ** -0.5, 0.09375, ((0, 8), (1, 4)))
    key_weight = bell_draw(key_list[3], (D, RET_WIDTH), D ** -0.5, 0.09375, ((0, 8), (1, 4)))
    value_weight = bell_draw(key_list[4], (D, RET_WIDTH), D ** -0.5, 0.09375, ((0, 8), (1, 4)))
    output_gate_weight = bell_draw(key_list[5], (D, RET_WIDTH), D ** -0.5, 0.09375, ((0, 8), (1, 4)))
    unit_input_weight = bell_draw(key_list[6], (D, CONV_WIDTH), D ** -0.5, 0.09375, ((0, 8), (1, 4)))
    unit_gate_weight = bell_draw(key_list[7], (D, CONV_WIDTH), D ** -0.5, 0.09375, ((0, 8), (1, 4)))
    decay_forward = draw_decay_forward(jax.random.fold_in(key_list[18], 71), 0)
    decay_backward = draw_decay_backward(jax.random.fold_in(key_list[18], 71), 0)
    group_gain = jnp.clip(1.0 + 0.18 * jax.random.normal(key_list[10], (RET_WIDTH,), jnp.float32), 0.1, 1.9)
    group_bias = bell_draw(key_list[11], (RET_WIDTH,), 0.5, 3.0, ((0, 4),), jnp.float32)
    depth_kernel = draw_depth_kernel(jax.random.fold_in(key_list[18], 71), 0)
    depth_bias = bell_draw(key_list[13], (CONV_WIDTH,), 0.5, 3.0, ((0, 4),), jnp.float32)
    channel_gain = jnp.clip(1.0 + 0.18 * jax.random.normal(key_list[14], (CONV_WIDTH,), jnp.float32), 0.1, 1.9)
    channel_bias = bell_draw(key_list[15], (CONV_WIDTH,), 0.5, 3.0, ((0, 4),), jnp.float32)
    retention_out_weight = bell_draw(key_list[16], (RET_WIDTH, D), (RET_WIDTH + CONV_WIDTH) ** -0.5, 0.09375, ((0, 4), (1, 8)))
    convolution_out_weight = bell_draw(key_list[17], (CONV_WIDTH, D), (RET_WIDTH + CONV_WIDTH) ** -0.5, 0.09375, ((0, 4), (1, 8)))
    return dict(hidden_states=hidden_states, norm_gain=norm_gain, query_weight=query_weight, key_weight=key_weight, value_weight=value_weight, output_gate_weight=output_gate_weight, unit_input_weight=unit_input_weight, unit_gate_weight=unit_gate_weight, decay_forward=decay_forward, decay_backward=decay_backward, group_gain=group_gain, group_bias=group_bias, depth_kernel=depth_kernel, depth_bias=depth_bias, channel_gain=channel_gain, channel_bias=channel_bias, retention_out_weight=retention_out_weight, convolution_out_weight=convolution_out_weight)


EPS = 1e-06
THETA = 10000.0

def rotate(rows, positions):
    half_dim = rows.shape[-1] // 2
    inverse = THETA ** (-jnp.arange(half_dim, dtype=jnp.float32) / half_dim)
    angles = positions.astype(jnp.float32)[:, None] * inverse[None, :]
    cosine = jnp.cos(angles)[:, None, :]
    sine = jnp.sin(angles)[:, None, :]
    widened = rows.astype(jnp.float32)
    first_half = widened[..., :half_dim]
    second_half = widened[..., half_dim:]
    turned = jnp.concatenate([first_half * cosine - second_half * sine, second_half * cosine + first_half * sine], axis=-1)
    return turned.astype(jnp.bfloat16)

def to_blocks(rows):
    return rows.reshape(rows.shape[0] // BLOCK, BLOCK, rows.shape[1], rows.shape[2]).transpose(2, 0, 1, 3)

def from_blocks(blocks):
    return blocks.transpose(1, 2, 0, 3).reshape(blocks.shape[1] * blocks.shape[2], blocks.shape[0], blocks.shape[3])

def blockwise(queries, key_rows, values, log_decay, include_diag):
    block_len = queries.shape[2]
    position = jnp.arange(block_len, dtype=jnp.float32)
    distance = position[:, None] - position[None, :]
    allowed = distance >= 0 if include_diag else distance > 0
    inside = jnp.where(allowed[None], jnp.exp(log_decay[:, None, None] * jnp.maximum(distance, 0.0)[None]), 0.0)
    query_wide = queries.astype(jnp.float32)
    key_wide = key_rows.astype(jnp.float32)
    value_wide = values.astype(jnp.float32)
    scores = jnp.einsum('hnqd,hnkd->hnqk', query_wide, key_wide, precision=lax.Precision.HIGHEST) * inside[:, None]
    inner_part = jnp.einsum('hnqk,hnkd->hnqd', scores, value_wide, precision=lax.Precision.HIGHEST)
    toward_end = jnp.exp(log_decay[:, None] * (block_len - 1.0 - position)[None])
    block_states = jnp.einsum('hnkd,hnke->hnde', key_wide * toward_end[:, None, :, None], value_wide, precision=lax.Precision.HIGHEST)
    block_decay = jnp.exp(log_decay * block_len)[:, None, None]

    def advance(state_now, block_state):
        return (block_decay * state_now + block_state, state_now)
    initial = jnp.zeros((block_states.shape[0], block_states.shape[2], block_states.shape[3]), jnp.float32)
    final_state, earlier = lax.scan(advance, initial, jnp.moveaxis(block_states, 1, 0))
    earlier = jnp.moveaxis(earlier, 0, 1)
    from_start = jnp.exp(log_decay[:, None] * (position + 1.0)[None])
    cross_part = jnp.einsum('hnqd,hnde->hnqe', query_wide * from_start[:, None, :, None], earlier, precision=lax.Precision.HIGHEST)
    return (inner_part + cross_part, final_state)

def group_norm(retained, group_gain, group_bias, gate_rows):
    row_mean = lax.optimization_barrier(jnp.mean(retained, axis=-1, keepdims=True))
    centered = retained - row_mean
    variance = lax.optimization_barrier(jnp.mean(centered * centered, axis=-1, keepdims=True))
    scaled = (centered * lax.rsqrt(variance + EPS)).reshape(retained.shape[0], -1)
    scaled = scaled * group_gain[None, :] + group_bias[None, :]
    return (jax.nn.silu(gate_rows.astype(jnp.float32)) * scaled).astype(jnp.bfloat16)

def reference(hidden_states, norm_gain, query_weight, key_weight, value_weight, output_gate_weight, unit_input_weight, unit_gate_weight, decay_forward, decay_backward, group_gain, group_bias, depth_kernel, depth_bias, channel_gain, channel_bias, retention_out_weight, convolution_out_weight):
    widened = hidden_states.astype(jnp.float32)
    normed = (widened * lax.rsqrt(lax.optimization_barrier(jnp.mean(widened * widened, axis=-1, keepdims=True)) + EPS) * norm_gain[None, :]).astype(jnp.bfloat16)

    def project(weight):
        return jnp.dot(normed, weight, preferred_element_type=jnp.float32).astype(jnp.bfloat16)
    proj_q = project(query_weight)
    proj_k = project(key_weight)
    proj_v = project(value_weight)
    proj_g = project(output_gate_weight)
    proj_a = project(unit_input_weight)
    proj_b = project(unit_gate_weight)
    positions = jnp.arange(TOKENS, dtype=jnp.int32)
    queries = rotate(proj_q.reshape(TOKENS, HEADS, HEAD_DIM), positions)
    key_rows = rotate(proj_k.reshape(TOKENS, HEADS, HEAD_DIM), positions)
    values = proj_v.reshape(TOKENS, HEADS, HEAD_DIM)
    log_forward = jax.nn.log_sigmoid(decay_forward)
    log_backward = jax.nn.log_sigmoid(decay_backward)
    ahead, unused_ahead = blockwise(to_blocks(queries), to_blocks(key_rows), to_blocks(values), log_forward, True)
    behind, unused_behind = blockwise(to_blocks(queries[::-1]), to_blocks(key_rows[::-1]), to_blocks(values[::-1]), log_backward, False)
    retained = from_blocks(ahead) + from_blocks(behind)[::-1]
    retention_rows = group_norm(retained, group_gain, group_bias, proj_g)
    unit = (proj_a.astype(jnp.float32) * jax.nn.sigmoid(proj_b.astype(jnp.float32))).astype(jnp.bfloat16)
    half_kernel = (KERNEL - 1) // 2
    padded = jnp.pad(unit, ((half_kernel, half_kernel), (0, 0)))
    filtered = jnp.broadcast_to(depth_bias[None, :], (TOKENS, CONV_WIDTH))
    for offset in range(KERNEL):
        filtered = filtered + depth_kernel[offset][None, :] * padded[offset:offset + TOKENS].astype(jnp.float32)
    row_mean = lax.optimization_barrier(jnp.sum(filtered, axis=1, keepdims=True)) / CONV_WIDTH
    variance = lax.optimization_barrier(jnp.sum(filtered * filtered, axis=1, keepdims=True)) / CONV_WIDTH - row_mean * row_mean
    leveled = (filtered - row_mean) * lax.rsqrt(variance + EPS) * channel_gain[None, :] + channel_bias[None, :]
    convolution_rows = jax.nn.silu(leveled).astype(jnp.bfloat16)
    ret_group = RET_WIDTH // N_TP
    conv_group = CONV_WIDTH // N_TP
    mixed = jnp.zeros((TOKENS, D), jnp.float32)
    for group in range(N_TP):
        partial_value = jnp.dot(retention_rows[:, group * ret_group:(group + 1) * ret_group], retention_out_weight[group * ret_group:(group + 1) * ret_group], preferred_element_type=jnp.float32)
        partial_value = partial_value + jnp.dot(convolution_rows[:, group * conv_group:(group + 1) * conv_group], convolution_out_weight[group * conv_group:(group + 1) * conv_group], preferred_element_type=jnp.float32)
        rounded = lax.optimization_barrier(partial_value.astype(jnp.bfloat16))
        mixed = mixed + rounded.astype(jnp.float32)
    return mixed.astype(jnp.bfloat16)
```

```python
import math

import jax
import jax.numpy as jnp
import numpy as np
from jax import lax
from jax.sharding import Mesh
from jax.sharding import PartitionSpec as P

HEAD_DIM = 128
EPS = 1e-06
THETA = 10000.0
F32 = jnp.float32
BF16 = jnp.bfloat16


def shifted(block, axis, shift):
    count = lax.axis_size(axis)
    return lax.ppermute(block, axis, [(i, (i + shift) % count) for i in range(count)])


def line_gather(block, axis):
    count = lax.axis_size(axis)
    index = lax.axis_index(axis)
    right, left = [block], [block]
    for step in range(1, count):
        right.append(
            lax.ppermute(right[-1], axis, [(i, i + 1) for i in range(step - 1, count - 1)])
        )
        left.append(
            lax.ppermute(left[-1], axis, [(i + 1, i) for i in range(0, count - step)])
        )
    return [block] + [
        jnp.where(index >= s, right[s], left[count - s]) for s in range(1, count)
    ]


def in_order(pieces, axis, dim):
    count = len(pieces)
    if count == 1:
        return pieces[0]
    index = lax.axis_index(axis)
    size = pieces[0].shape[dim]
    shape = list(pieces[0].shape)
    shape[dim] = size * count
    whole = jnp.zeros(shape, pieces[0].dtype)
    for s, piece in enumerate(pieces):
        whole = lax.dynamic_update_slice_in_dim(whole, piece, (index - s) % count * size, dim)
    return whole


def ring_gather(block, axis):
    return [block] + [shifted(block, axis, s) for s in range(1, lax.axis_size(axis))]


def fetch_columns(weights, width):
    count = lax.axis_size("n")
    index = lax.axis_index("n")

    def cut(dest):
        return jnp.concatenate(
            [lax.dynamic_slice_in_dim(w, dest * width, width, axis=1) for w in weights], axis=1
        )

    rows = [cut(index)] + [
        shifted(cut((index + s) % count), "n", s) for s in range(1, count)
    ]
    rows = [in_order(ring_gather(piece, "t"), "t", 0) for piece in rows]
    return in_order(rows, "n", 0)


def rotate(rows, positions):
    half_dim = rows.shape[-1] // 2
    inverse = THETA ** (-jnp.arange(half_dim, dtype=F32) / half_dim)
    angles = positions.astype(F32)[..., None] * inverse
    cosine, sine = jnp.cos(angles), jnp.sin(angles)
    widened = rows.astype(F32)
    first, second = widened[..., :half_dim], widened[..., half_dim:]
    turned = jnp.concatenate(
        [first * cosine - second * sine, second * cosine + first * sine], axis=-1
    )
    return turned.astype(BF16)


def retention(queries, keys, values, log_forward, log_backward):
    blocks, rows = queries.shape[:2]
    t_count, t_index = lax.axis_size("t"), lax.axis_index("t")
    place = jnp.arange(rows, dtype=F32)
    gap = place[:, None] - place[None, :]
    inside = jnp.exp(jnp.where(gap >= 0, log_forward * gap, -log_backward * gap))
    scores = jnp.einsum("nqd,nkd->nqk", queries, keys, preferred_element_type=F32) * inside
    local = jnp.einsum("nqk,nkd->nqd", scores.astype(BF16), values, preferred_element_type=F32)
    toward = jnp.stack(
        [jnp.exp(log_forward * (rows - 1.0 - place)), jnp.exp(log_backward * place)]
    )
    weighted = (keys.astype(F32)[None] * toward[:, None, :, None]).astype(BF16)
    states = jnp.einsum("snkd,nke->snde", weighted, values, preferred_element_type=F32).astype(
        BF16
    )
    gathered = jnp.stack(ring_gather(states, "t"), axis=2).astype(F32)
    source = (
        jnp.arange(blocks, dtype=jnp.int32)[:, None] * t_count
        + (t_index - jnp.arange(t_count, dtype=jnp.int32))[None, :] % t_count
    )
    target = jnp.arange(blocks, dtype=jnp.int32) * t_count + t_index
    ahead = (target[:, None, None] - source[None] - 1).astype(F32)
    behind = (source[None] - target[:, None, None] - 1).astype(F32)
    mix = jnp.stack(
        [
            jnp.where(ahead >= 0, jnp.exp(log_forward * rows * jnp.maximum(ahead, 0.0)), 0.0),
            jnp.where(behind >= 0, jnp.exp(log_backward * rows * jnp.maximum(behind, 0.0)), 0.0),
        ]
    )
    entering = jnp.einsum(
        "sbnt,sntde->sbde", mix, gathered, precision=lax.Precision.HIGHEST
    ).astype(BF16)
    lift = jnp.stack(
        [jnp.exp(log_forward * (place + 1.0)), jnp.exp(log_backward * (rows - place))]
    )
    carried = jnp.einsum("nqd,snde->snqe", queries, entering, preferred_element_type=F32)
    carried = carried * lift[:, None, :, None]
    return local + carried[0] + carried[1]


def halo(unit, width):
    t_count, t_index = lax.axis_size("t"), lax.axis_index("t")
    before = shifted(unit[:, -width:], "t", 1)
    after = shifted(unit[:, :width], "t", t_count - 1)
    edge = jnp.zeros_like(before[:1])
    before = jnp.where(t_index == 0, jnp.concatenate([edge, before[:-1]]), before)
    after = jnp.where(t_index == t_count - 1, jnp.concatenate([after[1:], edge]), after)
    return jnp.concatenate([before, unit, after], axis=1)


def shards(
    hidden_states,
    norm_gain,
    query_weight,
    key_weight,
    value_weight,
    output_gate_weight,
    unit_input_weight,
    unit_gate_weight,
    decay_forward,
    decay_backward,
    group_gain,
    group_bias,
    depth_kernel,
    depth_bias,
    channel_gain,
    channel_bias,
    retention_out_weight,
    convolution_out_weight,
):
    n_count, t_count = lax.axis_size("n"), lax.axis_size("t")
    x_count, c_count = lax.axis_size("x"), lax.axis_size("c")
    tp_count = x_count * c_count
    n_index, t_index = lax.axis_index("n"), lax.axis_index("t")
    x_index, c_index = lax.axis_index("x"), lax.axis_index("c")
    rows, features = hidden_states.shape
    model = norm_gain.shape[0]
    width = query_weight.shape[1] // n_count
    taps = depth_kernel.shape[0]
    conv_total = depth_bias.shape[0] * tp_count

    def own(vector):
        size = vector.shape[-1] // n_count
        return lax.dynamic_slice_in_dim(vector, n_index * size, size, axis=-1)

    widened = hidden_states.astype(F32)
    squares = lax.psum(jnp.sum(widened * widened, axis=-1), ("x", "c"))
    gain = lax.dynamic_slice_in_dim(
        norm_gain, (x_index * c_count + c_index) * features, features, axis=0
    )
    normed = (
        widened * lax.rsqrt(squares / model + EPS)[:, None] * gain[None, :]
    ).astype(BF16)

    unit_slab = fetch_columns((unit_input_weight, unit_gate_weight), width)
    keyval_slab = fetch_columns((key_weight, value_weight), width)
    query_slab = fetch_columns((query_weight, output_gate_weight), width)
    out_weight = jnp.concatenate([retention_out_weight, convolution_out_weight], axis=0)
    out_weight = in_order(ring_gather(out_weight, "t"), "t", 1)

    tokens = []
    for piece in line_gather(normed, "n"):
        piece = in_order(ring_gather(piece, "c"), "c", 1)
        tokens.append(in_order(ring_gather(piece, "x"), "x", 1))
    tokens = in_order(tokens, "n", 0)

    def project(slab):
        summed = jnp.dot(tokens, slab, preferred_element_type=F32).astype(BF16)
        summed = summed.reshape(n_count, rows, 2, width)
        return summed[:, :, 0], summed[:, :, 1]

    proj_a, proj_b = project(unit_slab)
    proj_k, proj_v = project(keyval_slab)
    proj_q, proj_g = project(query_slab)

    unit = (proj_a.astype(F32) * jax.nn.sigmoid(proj_b.astype(F32))).astype(BF16)
    padded = halo(unit, (taps - 1) // 2)
    kernel = own(depth_kernel)
    filtered = jnp.broadcast_to(own(depth_bias), unit.shape)
    for offset in range(taps):
        filtered = filtered + kernel[offset] * padded[:, offset : offset + rows].astype(F32)
    row_sum, row_squares = lax.psum(
        (jnp.sum(filtered, axis=-1), jnp.sum(filtered * filtered, axis=-1)), ("n", "x", "c")
    )
    row_mean = (row_sum / conv_total)[..., None]
    variance = (row_squares / conv_total)[..., None] - row_mean * row_mean
    leveled = (filtered - row_mean) * lax.rsqrt(variance + EPS) * own(channel_gain) + own(
        channel_bias
    )
    convolution_rows = jax.nn.silu(leveled).astype(BF16).reshape(n_count * rows, width)

    positions = (
        jnp.arange(n_count, dtype=jnp.int32)[:, None] * t_count + t_index
    ) * rows + jnp.arange(rows, dtype=jnp.int32)[None, :]
    retained = retention(
        rotate(proj_q, positions),
        rotate(proj_k, positions),
        proj_v,
        jax.nn.log_sigmoid(own(decay_forward))[0],
        jax.nn.log_sigmoid(own(decay_backward))[0],
    )
    mean = jnp.mean(retained, axis=-1, keepdims=True)
    centered = retained - mean
    spread = jnp.mean(centered * centered, axis=-1, keepdims=True)
    scaled = centered * lax.rsqrt(spread + EPS) * own(group_gain) + own(group_bias)
    retention_rows = (
        (jax.nn.silu(proj_g.astype(F32)) * scaled).astype(BF16).reshape(n_count * rows, width)
    )

    conv_all = in_order(line_gather(convolution_rows, "n"), "n", 1)
    ret_all = in_order(line_gather(retention_rows, "n"), "n", 1)
    half = retention_out_weight.shape[0]
    partial = jnp.dot(ret_all, out_weight[:half], preferred_element_type=F32) + jnp.dot(
        conv_all, out_weight[half:], preferred_element_type=F32
    )
    columns = partial.shape[-1]
    small = rows // tp_count
    partial = partial.astype(BF16).reshape(n_count, x_count, c_count, small, columns)

    def pick(stack, index, dim):
        return lax.dynamic_index_in_dim(stack, index, dim, keepdims=False)

    total = pick(partial, c_index, 2).astype(F32)
    for s in range(1, c_count):
        total = total + shifted(pick(partial, (c_index + s) % c_count, 2), "c", s).astype(F32)
    rounded = total.astype(BF16)
    total = pick(total, x_index, 1)
    for s in range(1, x_count):
        total = total + shifted(pick(rounded, (x_index + s) % x_count, 1), "x", s).astype(F32)
    rounded = total.astype(BF16)
    pieces = [pick(rounded, n_index, 0)] + [
        shifted(pick(rounded, (n_index + s) % n_count, 0), "n", s) for s in range(1, n_count)
    ]
    return in_order(pieces, "n", 1)


def solution(mesh):
    sp, tp = mesh.shape["sp"], mesh.shape["tp"]
    c_count = math.gcd(tp, 2)
    rows = ("n", "t")
    cols = ("x", "c")
    placed = (
        P(rows, cols),
        P(),
        P(rows, cols),
        P(rows, cols),
        P(rows, cols),
        P(rows, cols),
        P(rows, cols),
        P(rows, cols),
        P(cols),
        P(cols),
        P(cols),
        P(cols),
        P(None, cols),
        P(cols),
        P(cols),
        P(cols),
        P(cols, rows),
        P(cols, rows),
    )

    def program(*arrays):
        heads = arrays[2].shape[1] // HEAD_DIM // tp
        assert sp % heads == 0
        fine = Mesh(
            mesh.devices.reshape(heads, sp // heads, tp // c_count, c_count),
            ("n", "t", "x", "c"),
        )
        return jax.shard_map(
            shards,
            mesh=fine,
            in_specs=placed,
            out_specs=P(rows + cols, None),
            check_vma=False,
        )(*arrays)

    return program
```

```python
import functools
import math

import jax
import jax.numpy as jnp
import numpy as np
from jax import lax
from jax.experimental import pallas as pl
from jax.experimental.pallas import tpu as pltpu
from jax.sharding import Mesh
from jax.sharding import PartitionSpec as P


HEAD_DIM = 128
EPS = 1e-06
THETA = 10000.0
F32 = jnp.float32
BF16 = jnp.bfloat16

HALVES = 2
MIB = 1024 * 1024
GRANT = 67_000_000
HBM = pl.BlockSpec(memory_space=pltpu.HBM)
WHOLE = pl.BlockSpec(memory_space=pltpu.VMEM)


def shifted(block, axis, shift):
    count = lax.axis_size(axis)
    return lax.ppermute(block, axis, [(i, (i + shift) % count) for i in range(count)])


def ring_gather(block, axis):
    return [block] + [shifted(block, axis, s) for s in range(1, lax.axis_size(axis))]


def ring_sources(axis):
    count = lax.axis_size(axis)
    return [(lax.axis_index(axis) - s) % count for s in range(count)]


def pick_kernel(flag_ref, yes_ref, no_ref, out_ref, buf, in_sem, out_sem):
    parts = buf.shape[0]
    rows = buf.shape[1]

    def load(ref, k):
        return pltpu.make_async_copy(ref.at[pl.ds(k * rows, rows)], buf.at[k], in_sem.at[k])

    for k in range(parts):

        @pl.when(flag_ref[0] > 0)
        def _():
            load(yes_ref, k).start()

        @pl.when(flag_ref[0] <= 0)
        def _():
            load(no_ref, k).start()

    stores = [
        pltpu.make_async_copy(buf.at[k], out_ref.at[pl.ds(k * rows, rows)], out_sem.at[k])
        for k in range(parts)
    ]
    for k in range(parts):
        load(no_ref, k).wait()
        stores[k].start()
    for store in stores:
        store.wait()


def pick_call(flag, yes, no):
    rows, columns = yes.shape
    parts = 4
    return pl.pallas_call(
        pick_kernel,
        grid_spec=pltpu.PrefetchScalarGridSpec(
            num_scalar_prefetch=1,
            grid=(1,),
            in_specs=[HBM] * 2,
            out_specs=HBM,
            scratch_shapes=[
                pltpu.VMEM((parts, rows // parts, columns), BF16),
                pltpu.SemaphoreType.DMA((parts,)),
                pltpu.SemaphoreType.DMA((parts,)),
            ],
        ),
        out_shape=jax.ShapeDtypeStruct(yes.shape, yes.dtype),
        compiler_params=pltpu.CompilerParams(vmem_limit_bytes=GRANT),
        cost_estimate=cost(yes.size, 4 * yes.size),
    )(flag[None].astype(jnp.int32), yes, no)


def line_gather(block, axis):
    count = lax.axis_size(axis)
    index = lax.axis_index(axis)

    def move(value, pairs):
        return lax.ppermute(value, axis, pairs)

    if count == 4:
        ends = [(0, 1), (1, 0), (2, 3), (3, 2)]
        middle = [(1, 2), (2, 1)]
        outward = [(1, 0), (2, 3)]
        inner = (index == 1) | (index == 2)
        beside = move(block, ends)
        crossed = move(block, middle)
        second = move(beside, middle)
        passed = move(crossed, outward)
        last = move(second, outward)
        blocks = [block, beside, pick_call(inner, crossed, passed), pick_call(inner, second, last)]
        high = index >= 2
        owners = [
            index,
            index + 1 - 2 * (index % 2),
            jnp.where(high, 1, 2),
            jnp.where(high, 0, 3),
        ]
        return blocks, owners
    blocks = [block]
    for s in range(1, count):
        blocks.append(shifted(block, axis, s))
    return blocks, ring_sources(axis)


def cut_kernel(count, index_ref, *refs):
    buf, in_sem, out_sem = refs[-3:]
    width = buf.shape[-1]
    each = len(buf)
    weights, parts = refs[: each // count], refs[each // count : -3]
    loads, stores = [], []
    for k in range(each):
        column = pl.multiple_of(lax.rem(index_ref[0] + k % count, count) * width, 128)
        loads.append(
            pltpu.make_async_copy(
                weights[k // count].at[:, pl.ds(column, width)], buf.at[k], in_sem.at[k]
            )
        )
        loads[-1].start()
        stores.append(pltpu.make_async_copy(buf.at[k], parts[k], out_sem.at[k]))
    for load, store in zip(loads, stores):
        load.wait()
        store.start()
    for store in stores:
        store.wait()


def cut_call(weights, width):
    count = lax.axis_size("n")
    index = lax.axis_index("n")[None].astype(jnp.int32)
    rows = weights[0].shape[0]
    each = len(weights) * count
    parts = pl.pallas_call(
        functools.partial(cut_kernel, count),
        grid_spec=pltpu.PrefetchScalarGridSpec(
            num_scalar_prefetch=1,
            grid=(1,),
            in_specs=[HBM] * len(weights),
            out_specs=[HBM] * each,
            scratch_shapes=[
                pltpu.VMEM((each, rows, width), BF16),
                pltpu.SemaphoreType.DMA((each,)),
                pltpu.SemaphoreType.DMA((each,)),
            ],
        ),
        out_shape=[jax.ShapeDtypeStruct((rows, width), BF16)] * each,
        compiler_params=pltpu.CompilerParams(vmem_limit_bytes=GRANT),
        cost_estimate=cost(rows * width, 4 * rows * width * each),
    )(index, *weights)
    return [parts[k : k + count] for k in range(0, each, count)]


def stack_kernel(*refs):
    out_ref, buf, in_sem, out_sem = refs[-4:]
    loads, stores = [], []
    for k, ref in enumerate(refs[:-4]):
        loads.append(pltpu.make_async_copy(ref, buf.at[k], in_sem.at[k]))
        loads[-1].start()
        stores.append(pltpu.make_async_copy(buf.at[k], out_ref.at[k], out_sem.at[k]))
    for load, store in zip(loads, stores):
        load.wait()
        store.start()
    for store in stores:
        store.wait()


def stack_call(parts, label):
    shape = (len(parts),) + parts[0].shape
    return pl.pallas_call(
        stack_kernel,
        in_specs=[HBM] * len(parts),
        out_specs=HBM,
        scratch_shapes=[
            pltpu.VMEM(shape, BF16),
            pltpu.SemaphoreType.DMA((len(parts),)),
            pltpu.SemaphoreType.DMA((len(parts),)),
        ],
        out_shape=jax.ShapeDtypeStruct(shape, BF16),
        compiler_params=pltpu.CompilerParams(vmem_limit_bytes=2 * MIB if label[-1] in "qg" else GRANT),
        cost_estimate=cost(parts[0].size, 4 * len(parts) * parts[0].size),
    )(*parts)


def exchange(cuts, label):
    got = [cuts[0]] + [shifted(c, "n", s) for s, c in enumerate(cuts) if s]
    return stack_call(got, f"stack_{label}")


def cost(flops, moved):
    return pl.CostEstimate(flops=flops, bytes_accessed=moved, transcendentals=0)


def silu(x):
    return x * jax.nn.sigmoid(x)


def start_copies(idx_ref, t_offset, pieces, slabs, token_buf, slab_buf, piece_sem, slab_sem):
    tp_count, blocks = token_buf.shape[:2]
    n_count, rows, width = slabs[0].shape
    t_count = slab_buf.shape[0] // (n_count * rows)
    n_offset = t_offset + t_count
    slab_copies = []
    for m, slab in enumerate(slabs):
        for s in range(n_count):
            spot = idx_ref[n_offset + s] * t_count + idx_ref[t_offset + m % t_count]
            target = slab_buf.at[
                pl.ds(pl.multiple_of(spot * rows, rows), rows),
                pl.ds(m // t_count * width, width),
            ]
            slab_copies.append(
                pltpu.make_async_copy(slab.at[s], target, slab_sem.at[m * n_count + s])
            )
            slab_copies[-1].start()
    piece_copies = []
    for j in range(tp_count):
        piece_copies.append(
            [
                pltpu.make_async_copy(
                    pieces[k * tp_count + j],
                    token_buf.at[idx_ref[t_offset - tp_count + j], idx_ref[k]],
                    piece_sem.at[j, k],
                )
                for k in range(blocks)
            ]
        )
        for copy in piece_copies[-1]:
            copy.start()
    return slab_copies, piece_copies


def project(copies, token_buf, slab_buf, total_buf):
    slab_copies, piece_copies = copies
    tp_count, blocks, rows, features = token_buf.shape
    for copy in slab_copies:
        copy.wait()
    for waits in piece_copies:
        for copy in waits:
            copy.wait()
    for j in range(tp_count):
        part = jnp.dot(
            token_buf[j].reshape(blocks * rows, features),
            slab_buf[j * features : (j + 1) * features, :],
            preferred_element_type=F32,
        )
        if j == 0:
            total_buf[...] = part
        else:
            total_buf[...] += part


def project_scratch(blocks, tp_count, pieces, slabs, matrices):
    rows, features = pieces[0].shape
    n_count, _, width = slabs[0].shape
    model = features * tp_count
    return [
        pltpu.VMEM((model, matrices * width), BF16),
        pltpu.VMEM((tp_count, blocks, rows, features), BF16),
        pltpu.VMEM((blocks * rows, matrices * width), F32),
        pltpu.SemaphoreType.DMA((tp_count, blocks)),
        pltpu.SemaphoreType.DMA((len(slabs) * n_count,)),
    ]


def unit_kernel(t_offset, idx_ref, *refs):
    unit_ref, head_ref, tail_ref = refs[-8:-5]
    slab_buf, token_buf, total_buf, piece_sem, slab_sem = refs[-5:]
    count = token_buf.shape[0] * token_buf.shape[1]
    copies = start_copies(
        idx_ref, t_offset, refs[:count], refs[count:-8], token_buf, slab_buf, piece_sem, slab_sem
    )
    project(copies, token_buf, slab_buf, total_buf)
    blocks, rows, width = unit_ref.shape
    edge = head_ref.shape[1]
    both = total_buf[...].astype(BF16).astype(F32)
    unit = (both[:, :width] * jax.nn.sigmoid(both[:, width:])).astype(BF16)
    unit_ref[...] = unit.reshape(unit_ref.shape)
    for k in range(blocks):
        head_ref[k] = unit[k * rows : k * rows + edge]
        tail_ref[k] = unit[(k + 1) * rows - edge : (k + 1) * rows]


def unit_call(idx, t_offset, blocks, pieces, slabs, edge):
    tp_count = len(pieces) // blocks
    rows, features = pieces[0].shape
    width = slabs[0].shape[-1]
    return pl.pallas_call(
        functools.partial(unit_kernel, t_offset),
        grid_spec=pltpu.PrefetchScalarGridSpec(
            num_scalar_prefetch=1,
            grid=(1,),
            in_specs=[HBM] * (len(slabs) + len(pieces)),
            out_specs=[WHOLE] * 3,
            scratch_shapes=project_scratch(blocks, tp_count, pieces, slabs, 2),
        ),
        out_shape=[
            jax.ShapeDtypeStruct((blocks, rows, width), BF16),
            jax.ShapeDtypeStruct((blocks, edge, width), BF16),
            jax.ShapeDtypeStruct((blocks, edge, width), BF16),
        ],
        compiler_params=pltpu.CompilerParams(vmem_limit_bytes=GRANT),
        cost_estimate=cost(
            4 * blocks * rows * features * tp_count * width, blocks * rows * features * 8
        ),
        name="unit_0",
    )(idx, *pieces, *slabs)


def conv_kernel(t_offset, t_count, idx_ref, unit_ref, before_ref, after_ref, taps_ref, bias_ref, filtered_ref, sums_ref, buf):
    blocks, rows, width = unit_ref.shape
    base = before_ref.shape[1]
    reach = (taps_ref.shape[0] - 1) // 2
    t_index = idx_ref[t_offset]
    tile = min(rows, 64)
    ones = jnp.ones((8, width), F32)

    def step(block, carry):
        prev = jnp.where(t_index == 0, block - 1, block)
        succ = jnp.where(t_index == t_count - 1, block + 1, block)
        front = before_ref[jnp.maximum(prev, 0)].astype(F32)
        back = after_ref[jnp.minimum(succ, blocks - 1)].astype(F32)
        buf[:base, :] = jnp.where(prev >= 0, front, 0.0)
        buf[base : base + rows, :] = unit_ref[block].astype(F32)
        buf[base + rows :, :] = jnp.where(succ < blocks, back, 0.0)
        for start in range(0, rows, tile):
            total = jnp.broadcast_to(bias_ref[...], (tile, width))
            for offset in range(taps_ref.shape[0]):
                low = base - reach + start + offset
                total = total + taps_ref[offset : offset + 1, :] * buf[low : low + tile, :]
            filtered_ref[block, start : start + tile, :] = total
        whole = filtered_ref[block]
        for k, value in enumerate((whole, whole * whole)):
            summed = lax.dot_general(
                ones,
                value,
                (((1,), (1,)), ((), ())),
                precision=lax.Precision.HIGHEST,
                preferred_element_type=F32,
            )
            sums_ref[k, pl.ds(block, 1), :] = summed[:1]
        return carry

    lax.fori_loop(0, blocks, step, 0)


def conv_call(idx, t_offset, t_count, unit, before, after, taps, bias):
    blocks, rows, width = unit.shape
    return pl.pallas_call(
        functools.partial(conv_kernel, t_offset, t_count),
        grid_spec=pltpu.PrefetchScalarGridSpec(
            num_scalar_prefetch=1,
            grid=(1,),
            in_specs=[WHOLE] * 5,
            out_specs=[WHOLE] * 2,
            scratch_shapes=[pltpu.VMEM((rows + 2 * before.shape[1], width), F32)],
        ),
        out_shape=[
            jax.ShapeDtypeStruct((blocks, rows, width), F32),
            jax.ShapeDtypeStruct((2, blocks, rows), F32),
        ],
        compiler_params=pltpu.CompilerParams(vmem_limit_bytes=6 * MIB),
        cost_estimate=cost(10 * blocks * rows * width * 62, blocks * rows * width * 6),
        name="conv",
    )(idx, unit, before, after, taps, bias)


def level_kernel(total, filtered_ref, sums_ref, gain_ref, bias_ref, out_ref):
    blocks, _, width = filtered_ref.shape
    members = sums_ref.shape[0]
    ones = jnp.ones((members, width), F32)

    def step(block, carry):
        def whole(kind):
            return (
                lax.dot_general(
                    sums_ref[:, kind, block],
                    ones,
                    (((0,), (0,)), ((), ())),
                    precision=lax.Precision.HIGHEST,
                    preferred_element_type=F32,
                )
                / total
            )

        mean = whole(0)
        variance = whole(1) - mean * mean
        leveled = (filtered_ref[block] - mean) * lax.rsqrt(variance + EPS)
        leveled = leveled * gain_ref[...] + bias_ref[...]
        out_ref[block] = silu(leveled).astype(BF16)
        return carry

    lax.fori_loop(0, blocks, step, 0)


def level_call(total, filtered, sums, gain, bias):
    blocks, rows, width = filtered.shape
    return pl.pallas_call(
        functools.partial(level_kernel, total),
        in_specs=[WHOLE] * 4,
        out_specs=WHOLE,
        out_shape=jax.ShapeDtypeStruct((blocks, rows, width), BF16),
        compiler_params=pltpu.CompilerParams(vmem_limit_bytes=6 * MIB),
        cost_estimate=cost(40 * blocks * rows * width, blocks * rows * width * 6),
        name="level",
    )(filtered, sums, gain, bias)


def grows(rate, steps):
    return jnp.exp(rate * steps.astype(F32))


def keys_kernel(t_offset, idx_ref, rate_ref, near_ref, far_ref, *refs):
    parts_ref, state_ref, slab_buf, token_buf, total_buf, piece_sem, slab_sem = refs[-7:]
    count = token_buf.shape[0] * token_buf.shape[1]
    copies = start_copies(
        idx_ref, t_offset, refs[:count], refs[count:-7], token_buf, slab_buf, piece_sem, slab_sem
    )
    _, blocks, rows, width = parts_ref.shape
    place = lax.broadcasted_iota(jnp.int32, (rows, width), 0)
    sign = jnp.where(
        lax.broadcasted_iota(jnp.int32, (rows, width), 1) < width // 2, -1.0, 1.0
    )
    toward = (grows(rate_ref[0], rows - 1 - place), grows(rate_ref[1], place))
    project(copies, token_buf, slab_buf, total_buf)

    def step(block, carry):
        here = pl.ds(pl.multiple_of(block * rows, rows), rows)
        mixed = total_buf[here, :].astype(BF16)
        far_cos, far_sin = far_ref[0, pl.ds(block, 1), :], far_ref[1, pl.ds(block, 1), :]
        cosine = far_cos * near_ref[0] - far_sin * near_ref[1]
        sine = (far_sin * near_ref[0] + far_cos * near_ref[1]) * sign

        def turned(part):
            wide = part.astype(F32)
            return (wide * cosine + pltpu.roll(wide, width // 2, 1) * sine).astype(BF16)

        keys = turned(mixed[:, :width])
        values = mixed[:, width : 2 * width]
        parts_ref[0, block] = keys
        parts_ref[1, block] = values
        parts_ref[2, block] = turned(mixed[:, 2 * width : 3 * width])
        parts_ref[3, block] = mixed[:, 3 * width :]
        wide = keys.astype(F32)
        for way in range(2):
            weighted = (wide * toward[way]).astype(BF16)
            state_ref[way, block] = lax.dot_general(
                weighted, values, (((0,), (0,)), ((), ())), preferred_element_type=F32
            ).astype(BF16)
        return carry

    lax.fori_loop(0, blocks, step, 0)


def keys_call(idx, rates, t_offset, blocks, near, far, pieces, slabs):
    tp_count = len(pieces) // blocks
    rows, features = pieces[0].shape
    width = slabs[0].shape[-1]
    return pl.pallas_call(
        functools.partial(keys_kernel, t_offset),
        grid_spec=pltpu.PrefetchScalarGridSpec(
            num_scalar_prefetch=2,
            grid=(1,),
            in_specs=[WHOLE] * 2 + [HBM] * (len(slabs) + len(pieces)),
            out_specs=[WHOLE] * 2,
            scratch_shapes=project_scratch(blocks, tp_count, pieces, slabs, 4),
        ),
        out_shape=[
            jax.ShapeDtypeStruct((4, blocks, rows, width), BF16),
            jax.ShapeDtypeStruct((2, blocks, width, width), BF16),
        ],
        compiler_params=pltpu.CompilerParams(vmem_limit_bytes=GRANT),
        cost_estimate=cost(
            8 * blocks * rows * features * tp_count * width, blocks * rows * features * 8
        ),
        name="keys",
    )(idx, rates, near, far, *pieces, *slabs)


def local_kernel(rate_ref, parts_ref, local_ref, inside_buf):
    rows = local_ref.shape[1]
    square = (rows, rows)

    @pl.when(pl.program_id(0) == 0)
    def _():
        gap = lax.broadcasted_iota(jnp.int32, square, 0) - lax.broadcasted_iota(
            jnp.int32, square, 1
        )
        inside_buf[...] = jnp.exp(
            jnp.where(gap >= 0, rate_ref[0], -rate_ref[1]) * gap.astype(F32)
        )

    scores = lax.dot_general(
        parts_ref[2, 0], parts_ref[0, 0], (((1,), (1,)), ((), ())), preferred_element_type=F32
    )
    scores = (scores * inside_buf[...]).astype(BF16)
    local_ref[0] = jnp.dot(scores, parts_ref[1, 0], preferred_element_type=F32)


def local_call(rates, parts):
    _, blocks, rows, width = parts.shape
    return pl.pallas_call(
        local_kernel,
        grid_spec=pltpu.PrefetchScalarGridSpec(
            num_scalar_prefetch=1,
            grid=(blocks,),
            in_specs=[pl.BlockSpec((3, 1, rows, width), lambda b, at: (0, b, 0, 0))],
            out_specs=pl.BlockSpec((1, rows, width), lambda b, at: (b, 0, 0)),
            scratch_shapes=[pltpu.VMEM((rows, rows), F32)],
        ),
        out_shape=jax.ShapeDtypeStruct((blocks, rows, width), F32),
        compiler_params=pltpu.CompilerParams(vmem_limit_bytes=4 * MIB),
        cost_estimate=cost(4 * blocks * rows * rows * width, 10 * blocks * rows * width),
        name="local",
    )(rates, parts)


def cross_kernel(
    t_offset, idx_ref, rate_ref, local_ref, parts_ref, gain_ref, bias_ref, *refs
):
    outs = refs[-2 - HALVES : -2]
    state_buf, enter_buf = refs[-2:]
    states = refs[: -2 - HALVES]
    blocks, rows, width = local_ref.shape
    t_count = len(states)
    total = blocks * t_count
    t_index = idx_ref[t_offset]
    for t, state in enumerate(states):
        for way in range(2):
            for source in range(blocks):
                state_buf[way, source * t_count + idx_ref[t_offset + t]] = state[
                    way, source
                ].astype(F32)
    size = jnp.full((width, width), rows, jnp.int32)
    for way in range(2):
        fade = grows(rate_ref[way], size)

        def advance(k, entering, way=way, fade=fade):
            block = k if way == 0 else total - 1 - k

            @pl.when(block % t_count == t_index)
            def _():
                enter_buf[way, block // t_count] = entering.astype(BF16)

            return entering * fade + state_buf[way, block]

        lax.fori_loop(0, total, advance, jnp.zeros((width, width), F32))
    place = lax.broadcasted_iota(jnp.int32, (rows, width), 0)
    lift = (grows(rate_ref[0], place + 1), grows(rate_ref[1], rows - place))

    def step(block, carry):
        retained = local_ref[block]
        for way in range(2):
            carried = jnp.dot(
                parts_ref[2, block], enter_buf[way, block], preferred_element_type=F32
            )
            retained = retained + carried * lift[way]
        centered = retained - jnp.mean(retained, axis=-1, keepdims=True)
        spread = jnp.mean(centered * centered, axis=-1, keepdims=True)
        scaled = centered * lax.rsqrt(spread + EPS) * gain_ref[...] + bias_ref[...]
        done = (silu(parts_ref[3, block].astype(F32)) * scaled).astype(BF16)
        tp_count, small = outs[0].shape[1:3]
        done = done.reshape(tp_count, HALVES, small, width)
        for half in range(HALVES):
            outs[half][block] = done[:, half]
        return carry

    lax.fori_loop(0, blocks, step, 0)


def cross_call(idx, rates, t_offset, tp_count, local, parts, gain, bias, states):
    blocks, rows, width = local.shape
    small = rows // tp_count // HALVES
    return pl.pallas_call(
        functools.partial(cross_kernel, t_offset),
        grid_spec=pltpu.PrefetchScalarGridSpec(
            num_scalar_prefetch=2,
            grid=(1,),
            in_specs=[WHOLE] * (4 + len(states)),
            out_specs=[WHOLE] * HALVES,
            scratch_shapes=[
                pltpu.VMEM((2, blocks * len(states), width, width), F32),
                pltpu.VMEM((2, blocks, width, width), BF16),
            ],
        ),
        out_shape=[jax.ShapeDtypeStruct((blocks, tp_count, small, width), BF16)] * HALVES,
        compiler_params=pltpu.CompilerParams(vmem_limit_bytes=8 * MIB),
        cost_estimate=cost(60 * blocks * rows * width, blocks * rows * width * 10),
        name="cross",
    )(idx, rates, local, parts, gain, bias, *states)


def out_kernel(n_count, c_count, t_offset, idx_ref, *refs):
    outs, side_buf = refs[-1 - c_count : -1], refs[-1]
    weights = refs[2 * n_count : -1 - c_count]
    count = len(weights) // 2
    width = refs[0].shape[-1]
    n_offset = t_offset + count
    c_offset = n_offset + n_count
    shape = outs[0].shape
    rows = shape[0] * shape[1]
    for k, ref in enumerate(refs[: 2 * n_count]):
        column = pl.multiple_of(idx_ref[n_offset + k % n_count] * width, width)
        for c in range(c_count):
            part = ref[:, :, pl.ds(idx_ref[c_offset + c], 1)].reshape(rows, width)
            side_buf[k // n_count, c * rows : (c + 1) * rows, pl.ds(column, width)] = part
    for s in range(count):
        summed = sum(
            jnp.dot(side_buf[k], weights[k * count + s][...], preferred_element_type=F32)
            for k in range(2)
        ).astype(BF16)
        size = summed.shape[1]
        column = pl.multiple_of(idx_ref[t_offset + s] * size, 128)
        for c in range(c_count):
            part = summed[c * rows : (c + 1) * rows].reshape(shape[:2] + (size,))
            outs[c][:, :, pl.ds(column, size)] = part


def out_call(idx, t_offset, half, rets, convs, ret_weights, conv_weights):
    n_count = len(rets)
    blocks, x_count, c_count, rows, width = rets[0].shape
    depth, size = ret_weights[0].shape
    total = size * len(ret_weights)
    conv_spec = pl.BlockSpec(
        (blocks, x_count, c_count, 1, rows, width), lambda b, idx: (0, 0, 0, half, 0, 0)
    )
    outs = pl.pallas_call(
        functools.partial(out_kernel, n_count, c_count, t_offset),
        grid_spec=pltpu.PrefetchScalarGridSpec(
            num_scalar_prefetch=1,
            grid=(1,),
            in_specs=[WHOLE] * n_count
            + [conv_spec] * n_count
            + [WHOLE] * (2 * len(ret_weights)),
            out_specs=[WHOLE] * c_count,
            scratch_shapes=[
                pltpu.VMEM((2, c_count * blocks * x_count * rows, n_count * width), BF16)
            ],
        ),
        out_shape=[jax.ShapeDtypeStruct((blocks, x_count * rows, total), BF16)] * c_count,
        compiler_params=pltpu.CompilerParams(vmem_limit_bytes=16 * MIB),
        cost_estimate=cost(
            4 * blocks * x_count * c_count * rows * depth * total, 4 * depth * total
        ),
    )(idx, *rets, *convs, *ret_weights, *conv_weights)
    return [out.reshape(blocks, x_count, rows, total) for out in outs]


def fold_c_kernel(offset, idx_ref, *refs):
    x_count = refs[0].shape[1]
    parts, outs = refs[:-x_count], refs[-x_count:]
    for s, out in enumerate(outs):
        x = idx_ref[offset + s]
        total = parts[0][:, x].astype(F32)
        for part in parts[1:]:
            total = total + part[:, x].astype(F32)
        out[...] = total.astype(out.dtype)


def fold_c_call(idx, offset, parts):
    blocks, x_count, rows, columns = parts[0].shape
    return pl.pallas_call(
        functools.partial(fold_c_kernel, offset),
        grid_spec=pltpu.PrefetchScalarGridSpec(
            num_scalar_prefetch=1,
            grid=(1,),
            in_specs=[WHOLE] * len(parts),
            out_specs=[WHOLE] * x_count,
        ),
        out_shape=[
            jax.ShapeDtypeStruct((blocks, rows, columns), BF16 if s else F32)
            for s in range(x_count)
        ],
        compiler_params=pltpu.CompilerParams(vmem_limit_bytes=8 * MIB),
        cost_estimate=cost(parts[0].size * len(parts), parts[0].size * 6),
    )(idx, *parts)


def fold_x_kernel(offset, idx_ref, *refs):
    count = refs[0].shape[0]
    parts, outs = refs[:-count], refs[-count:]
    for s, out in enumerate(outs):
        n = idx_ref[offset + s]
        total = parts[0][n]
        for part in parts[1:]:
            total = total + part[n].astype(F32)
        out[...] = total.astype(BF16)


def fold_x_call(idx, offset, parts):
    blocks, rows, columns = parts[0].shape
    return pl.pallas_call(
        functools.partial(fold_x_kernel, offset),
        grid_spec=pltpu.PrefetchScalarGridSpec(
            num_scalar_prefetch=1,
            grid=(1,),
            in_specs=[WHOLE] * len(parts),
            out_specs=[WHOLE] * blocks,
        ),
        out_shape=[jax.ShapeDtypeStruct((rows, columns), BF16)] * blocks,
        compiler_params=pltpu.CompilerParams(vmem_limit_bytes=4 * MIB),
        cost_estimate=cost(parts[0].size * len(parts), parts[0].size * 8),
    )(idx, *parts)


def turn_tables(starts, rows, width):
    half = width // 2
    inverse = THETA ** (-np.arange(half, dtype=np.float64) / half)
    inverse = np.concatenate([inverse, inverse])
    near = np.arange(rows, dtype=np.float64)[:, None] * inverse[None, :]
    near = jnp.asarray(np.stack([np.cos(near), np.sin(near)]), F32)
    far = starts.astype(F32)[:, None] * jnp.asarray(inverse, F32)[None, :]
    return near, jnp.stack([jnp.cos(far), jnp.sin(far)])


def spread_rows(copies, axis):
    return lax.all_to_all(copies, axis, 0, 0, tiled=True)


def small_tables(
    n_index, t_index, n_count, t_count, rows, width, taps, kernel, *vectors_and_decays
):
    vectors = vectors_and_decays[:-2]
    stacked = jnp.concatenate([kernel] + [v[None] for v in vectors])
    stacked = lax.dynamic_slice_in_dim(stacked, n_index * width, width, axis=1)
    decay = jax.nn.log_sigmoid(jnp.stack(vectors_and_decays[-2:]))
    rates = lax.dynamic_slice_in_dim(decay, n_index, 1, axis=1)[:, 0]
    starts = (jnp.arange(n_count, dtype=jnp.int32) * t_count + t_index) * rows
    near, far = turn_tables(starts, rows, width)
    rows_of = [stacked[taps + k : taps + k + 1] for k in range(len(vectors))]
    return stacked[:taps], rows_of, rates, near, far


def shards(
    hidden_states,
    norm_gain,
    query_weight,
    key_weight,
    value_weight,
    output_gate_weight,
    unit_input_weight,
    unit_gate_weight,
    decay_forward,
    decay_backward,
    group_gain,
    group_bias,
    depth_kernel,
    depth_bias,
    channel_gain,
    channel_bias,
    retention_out_weight,
    convolution_out_weight,
):
    n_count, t_count = lax.axis_size("n"), lax.axis_size("t")
    x_count, c_count = lax.axis_size("x"), lax.axis_size("c")
    tp_count = x_count * c_count
    n_index, t_index = lax.axis_index("n"), lax.axis_index("t")
    x_index, c_index = lax.axis_index("x"), lax.axis_index("c")
    rows = hidden_states.shape[0]
    width = query_weight.shape[1] // n_count
    taps = depth_kernel.shape[0]
    conv_total = depth_bias.shape[0] * tp_count

    half = (taps - 1) // 2
    kernel, rows_of, rates, near, far = small_tables(
        n_index, t_index, n_count, t_count, rows, width, taps,
        depth_kernel, depth_bias, channel_gain, channel_bias, group_gain, group_bias,
        decay_forward, decay_backward,
    )
    conv_bias, conv_gain, conv_shift, ret_gain, ret_shift = rows_of

    weights = {
        "a": unit_input_weight,
        "b": unit_gate_weight,
        "k": key_weight,
        "v": value_weight,
        "q": query_weight,
        "g": output_gate_weight,
    }
    slabs = {}
    for names in ("ab", "kvqg"):
        cuts = cut_call([weights[name] for name in names], width)
        for name, cut in zip(names, cuts):
            slabs[name] = ring_gather(exchange(cut, f"swap_{name}"), "t")
    ret_weights = ring_gather(retention_out_weight, "t")
    conv_weights = ring_gather(convolution_out_weight, "t")

    features = hidden_states.shape[1]
    widened = hidden_states.astype(F32)
    squares = lax.psum(jnp.sum(widened * widened, axis=-1), ("x", "c"))
    gain = lax.dynamic_slice_in_dim(
        norm_gain, (x_index * c_count + c_index) * features, features, axis=0
    )
    scale = lax.rsqrt(squares / norm_gain.shape[0] + EPS)
    normed = (widened * scale[:, None] * gain[None, :]).astype(BF16)
    blocks, owners = line_gather(normed, "n")
    pieces = []
    for block in blocks:
        for side in ring_gather(block, "x"):
            pieces += ring_gather(side, "c")
    columns = [x * c_count + c for x in ring_sources("x") for c in ring_sources("c")]
    idx = jnp.stack(
        owners
        + columns
        + ring_sources("t")
        + ring_sources("n")
        + ring_sources("c")
        + [(x_index + s) % x_count for s in range(x_count)]
        + [(n_index + s) % n_count for s in range(n_count)]
    ).astype(jnp.int32)
    t_offset = n_count + tp_count
    c_offset = t_offset + t_count + n_count
    x_offset = c_offset + c_count

    edge = -(-half // 16) * 16
    unit_slabs = slabs["a"] + slabs["b"]
    unit, head, tail = unit_call(idx, t_offset, n_count, pieces, unit_slabs, edge)

    before = shifted(tail, "t", 1)
    after = shifted(head, "t", t_count - 1)
    filtered, sums = conv_call(idx, t_offset, t_count, unit, before, after, kernel, conv_bias)
    members = n_count * tp_count
    sums = jnp.broadcast_to(sums[None], (members,) + sums.shape)
    sums = spread_rows(sums, ("n", "x", "c"))
    convolved = level_call(conv_total, filtered, sums, conv_gain, conv_shift)
    small = rows // tp_count // HALVES
    convs = [
        c.reshape(n_count, x_count, c_count, HALVES, small, width)
        for c in ring_gather(convolved, "n")
    ]

    every = slabs["k"] + slabs["v"] + slabs["q"] + slabs["g"]
    parts, states = keys_call(idx, rates, t_offset, n_count, near, far, pieces, every)
    local = local_call(rates, parts)
    gated = cross_call(
        idx,
        rates,
        t_offset,
        tp_count,
        local,
        parts,
        ret_gain,
        ret_shift,
        ring_gather(states, "t"),
    )
    mixed = []
    for half in range(HALVES):
        mine = gated[half].reshape(n_count, x_count, c_count, small, width)
        rets = ring_gather(mine, "n")
        parts = out_call(idx, t_offset, half, rets, convs, ret_weights, conv_weights)
        for s in range(1, c_count):
            parts[s] = shifted(parts[s], "c", c_count - s)
        shares = list(fold_c_call(idx, x_offset, parts))
        for s in range(1, x_count):
            shares[s] = shifted(shares[s], "x", s)
        pieces = fold_x_call(idx, x_offset + x_count, shares)
        mixed.append(pieces[0])
        for s in range(1, n_count):
            mixed.append(shifted(pieces[s], "n", s))
    return join_call(jnp.stack(ring_sources("n")).astype(jnp.int32), mixed)


def join_kernel(order_ref, *refs):
    rows, size = refs[0].shape
    each = (len(refs) - 1) // HALVES
    for k, piece in enumerate(refs[:-1]):
        column = pl.multiple_of(order_ref[k % each] * size, 128)
        refs[-1][k // each * rows : (k // each + 1) * rows, pl.ds(column, size)] = piece[...]


def join_call(order, pieces):
    rows, size = pieces[0].shape
    shape = (rows * HALVES, size * (len(pieces) // HALVES))
    return pl.pallas_call(
        join_kernel,
        grid_spec=pltpu.PrefetchScalarGridSpec(
            num_scalar_prefetch=1,
            grid=(1,),
            in_specs=[WHOLE] * len(pieces),
            out_specs=WHOLE,
        ),
        out_shape=jax.ShapeDtypeStruct(shape, BF16),
        compiler_params=pltpu.CompilerParams(vmem_limit_bytes=4 * MIB),
        cost_estimate=cost(rows * size, 4 * rows * size * len(pieces)),
        name="join",
    )(order, *pieces)


def solution(mesh):
    sp, tp = mesh.shape["sp"], mesh.shape["tp"]
    c_count = math.gcd(tp, 2)
    rows = ("n", "t")
    cols = ("x", "c")
    placed = (
        P(rows, cols),
        P(),
        P(rows, cols),
        P(rows, cols),
        P(rows, cols),
        P(rows, cols),
        P(rows, cols),
        P(rows, cols),
        P(cols),
        P(cols),
        P(cols),
        P(cols),
        P(None, cols),
        P(cols),
        P(cols),
        P(cols),
        P(cols, rows),
        P(cols, rows),
    )

    def program(*arrays):
        heads = arrays[2].shape[1] // HEAD_DIM // tp
        assert sp % heads == 0
        fine = Mesh(
            mesh.devices.reshape(heads, sp // heads, tp // c_count, c_count),
            ("n", "t", "x", "c"),
        )

        mapped = jax.shard_map(
            shards,
            mesh=fine,
            in_specs=placed,
            out_specs=P(rows + cols, None),
            check_vma=False,
        )
        return mapped(*arrays)

    return program
```
